32 devices in a mesh: sp: 8 (over z, y), tp: 4 (over x, core).
Axes of the slice: x: 2, y: 2, z: 4, core: 2. Of those that a mesh axis runs over, the one named last changes fastest.
Arguments:
- latent: bfloat16 [2048, 2048], P('sp'), may hold values from -6 to 6
- context: bfloat16 [1024, 2048], P('sp'), may hold values from -6 to 6
- condition: bfloat16 [2048], replicated, may hold values from -6 to 6
- context_condition: bfloat16 [2048], replicated, may hold values from -6 to 6
- gain_pre: float32 [2048], replicated, may hold values from 0.1 to 1.9
- gain_post: float32 [2048], replicated, may hold values from 0.1 to 1.9
- w_shift: bfloat16 [2048, 2048], P('sp', 'tp'), may hold values from -0.125 to 0.125
- w_scale: bfloat16 [2048, 2048], P('sp', 'tp'), may hold values from -0.125 to 0.125
- w_gate: bfloat16 [2048, 2048], P('sp', 'tp'), may hold values from -0.125 to 0.125
- w_query: bfloat16 [2048, 2048], P(None, 'tp'), may hold values from -0.13258252 to 0.13258252
- w_key: bfloat16 [2048, 2048], P(None, 'tp'), may hold values from -6.629126 to 6.629126
- w_value: bfloat16 [2048, 2048], P(None, 'tp'), may hold values from -0.125 to 0.125
- w_silu: bfloat16 [2048, 2048], P(None, 'tp'), may hold values from -0.125 to 0.125
- offset_bias: float32 [32, 15, 31], P('tp'), may hold values from 1.5 to 3.5
- w_out: bfloat16 [2048, 2048], P('tp'), may hold values from -0.125 to 0.125
Outputs:
- updated: bfloat16 [2048, 2048], P(('sp', 'tp'))
The draws below stay inside these ranges and needn't reach their ends.
All inputs are finite; a program needn't handle non-finite values.
Results may differ from the reference program's by a relative error of at most 0.01.
Values may be sent and summed in bfloat16 or wider, within the bound.
A program may use at most 64 MiB of HBM per device.

```python
import jax
import jax.numpy as jnp
from jax import lax

D = 2048
HEADS = 32
HEAD_DIM = 64
GRID_W = 64
WIN_ROWS = 8
WIN_COLS = 16
CTX = 1024
TOKENS = 2048
N_TP = 4


def query_key_pair(key):
    base = jax.random.fold_in(key, 7)
    first, second, third = jax.random.split(base, 3)
    spread = D ** (-0.5)
    weight_query = jnp.clip(jax.random.normal(first, (D, D), jnp.float32), -6.0, 6.0) * spread
    weight_key = jnp.clip(jax.random.normal(second, (D, D), jnp.float32), -6.0, 6.0) * spread
    return (weight_query, weight_key)


def draw_w_query(key, part):
    return query_key_pair(key)[0].astype(jnp.bfloat16)


def draw_w_key(key, part):
    return query_key_pair(key)[1].astype(jnp.bfloat16)


def steps_of(key, dims, pieces, smallest, high):
    def one(dim, shards_of):
        steps = jax.random.uniform(jax.random.fold_in(jax.random.fold_in(key, 6), dim), (shards_of,), jnp.float32, smallest / len(pieces), high / len(pieces))
        return jnp.repeat(jnp.exp(steps), dims[dim] // shards_of).reshape((-1,) + (1,) * (len(dims) - dim - 1))

    factor_of = one(*pieces[0])
    for cut in pieces[1:]:
        factor_of = factor_of * one(*cut)
    return factor_of


def scatter_about(stream_key, dims, scale, reach, cuts=(), kind=jnp.bfloat16):
    factor_of = steps_of(stream_key, dims, cuts, -0.22, 0.18) if cuts else 1.0
    values = jax.random.normal(stream_key, dims, jnp.float32) * scale * factor_of
    return jnp.minimum(jnp.maximum(values, -reach), reach).astype(kind)


def setup_inputs(seed: int = 0) -> dict:
    streams_of = jax.random.split(jax.random.key(seed), 16)
    latent = scatter_about(streams_of[0], (TOKENS, D), 1.0, 6.0, ((0, 8),))
    context = scatter_about(streams_of[1], (CTX, D), 1.0, 6.0, ((0, 8),))
    condition = scatter_about(streams_of[2], (D,), 1.0, 6.0)
    context_condition = scatter_about(streams_of[3], (D,), 1.0, 6.0)
    gain_pre = jnp.clip(1.0 + 0.18 * jax.random.normal(streams_of[4], (D,), jnp.float32), 0.1, 1.9)
    gain_post = jnp.clip(1.0 + 0.18 * jax.random.normal(streams_of[5], (D,), jnp.float32), 0.1, 1.9)
    w_shift = scatter_about(streams_of[6], (D, D), D ** -0.5, 0.125, ((0, 8), (1, 4)))
    w_scale = scatter_about(streams_of[7], (D, D), D ** -0.5, 0.125, ((0, 8), (1, 4)))
    w_gate = scatter_about(streams_of[8], (D, D), D ** -0.5, 0.125, ((0, 8), (1, 4)))
    w_query = draw_w_query(jax.random.fold_in(streams_of[15], 71), 0)
    w_key = draw_w_key(jax.random.fold_in(streams_of[15], 71), 0)
    w_value = scatter_about(streams_of[11], (D, D), D ** -0.5, 0.125, ((1, 4),))
    w_silu = scatter_about(streams_of[12], (D, D), D ** -0.5, 0.125, ((1, 4),))
    offset_bias = jnp.clip(1.5 + 2.0 * jax.random.uniform(streams_of[13], (HEADS, 2 * WIN_ROWS - 1, 2 * WIN_COLS - 1), jnp.float32) ** steps_of(streams_of[13], (HEADS, 2 * WIN_ROWS - 1, 2 * WIN_COLS - 1), ((0, 4),), -0.2, 0.2), 1.5, 3.5)
    w_out = scatter_about(streams_of[14], (D, D), D ** -0.5, 0.125, ((0, 4),))
    return {"latent": latent, "context": context, "condition": condition, "context_condition": context_condition, "gain_pre": gain_pre, "gain_post": gain_post, "w_shift": w_shift, "w_scale": w_scale, "w_gate": w_gate, "w_query": w_query, "w_key": w_key, "w_value": w_value, "w_silu": w_silu, "offset_bias": offset_bias, "w_out": w_out}


EPSILON = 1e-06

def rounded(values):
    return lax.optimization_barrier(values.astype(jnp.bfloat16))

def normalize(row_block, gain_row):
    values = row_block.astype(jnp.float32)
    return values * lax.rsqrt(lax.optimization_barrier(jnp.mean(values * values, axis=-1, keepdims=True)) + EPSILON) * gain_row

def project(row_block, weight):
    return rounded(jnp.dot(row_block, weight, preferred_element_type=jnp.float32))

def reference(latent, context, condition, context_condition, gain_pre, gain_post, w_shift, w_scale, w_gate, w_query, w_key, w_value, w_silu, offset_bias, w_out):
    active = jax.nn.silu(jnp.stack([condition, context_condition]).astype(jnp.float32)).astype(jnp.bfloat16)
    shifts = jnp.dot(active, w_shift, preferred_element_type=jnp.float32)
    scales = jnp.dot(active, w_scale, preferred_element_type=jnp.float32)
    gating = jnp.dot(active, w_gate, preferred_element_type=jnp.float32)
    hidden = rounded(normalize(latent, gain_pre) * (1.0 + scales[0]) + shifts[0])
    context_hidden = rounded(normalize(context, gain_pre) * (1.0 + scales[1]) + shifts[1])
    queries = project(hidden, w_query)
    keys_latent = project(hidden, w_key)
    values_latent = project(hidden, w_value)
    silu_gate = project(hidden, w_silu)
    context_keys = project(context_hidden, w_key).reshape(-1, HEADS, HEAD_DIM).astype(jnp.float32)
    context_values = project(context_hidden, w_value).reshape(-1, HEADS, HEAD_DIM).astype(jnp.float32)
    tokens, model_width = latent.shape
    grid_rows = tokens // GRID_W
    score_scale = HEAD_DIM ** (-0.5)
    query_grid = queries.reshape(grid_rows, GRID_W, HEADS, HEAD_DIM)
    key_grid = keys_latent.reshape(grid_rows, GRID_W, HEADS, HEAD_DIM)
    value_grid = values_latent.reshape(grid_rows, GRID_W, HEADS, HEAD_DIM)
    columns = jnp.arange(GRID_W, dtype=jnp.int32)
    col_start = jnp.clip(columns - WIN_COLS // 2, 0, GRID_W - WIN_COLS)
    col_inside = (columns[None, :] >= col_start[:, None]) & (columns[None, :] < col_start[:, None] + WIN_COLS)
    col_offset = jnp.clip(columns[None, :] - columns[:, None] + WIN_COLS - 1, 0, 2 * WIN_COLS - 2)

    def row_step(row_index):
        row_first = jnp.clip(row_index - WIN_ROWS // 2, 0, grid_rows - WIN_ROWS)
        query_row = lax.dynamic_index_in_dim(query_grid, row_index, 0, keepdims=False).astype(jnp.float32)
        key_band = lax.dynamic_slice_in_dim(key_grid, row_first, WIN_ROWS, 0).astype(jnp.float32)
        value_band = lax.dynamic_slice_in_dim(value_grid, row_first, WIN_ROWS, 0).astype(jnp.float32)
        row_offset = row_first + jnp.arange(WIN_ROWS, dtype=jnp.int32) - row_index + WIN_ROWS - 1
        offset_terms = offset_bias[:, row_offset[:, None, None], col_offset[None, :, :]]
        window_scores = jnp.einsum('qhd,vkhd->hqvk', query_row, key_band) * score_scale + jnp.transpose(offset_terms, (0, 2, 1, 3))
        window_scores = jnp.where(col_inside[None, :, None, :], window_scores, -jnp.inf)
        context_scores = jnp.einsum('qhd,jhd->hqj', query_row, context_keys) * score_scale
        maximum = jnp.maximum(lax.optimization_barrier(jnp.max(window_scores, axis=(2, 3))), lax.optimization_barrier(jnp.max(context_scores, axis=2)))
        window_exp = jnp.exp(window_scores - maximum[:, :, None, None])
        context_exp = jnp.exp(context_scores - maximum[:, :, None])
        denominator = lax.optimization_barrier(jnp.sum(window_exp, axis=(2, 3))) + lax.optimization_barrier(jnp.sum(context_exp, axis=2))
        window_weights = rounded(window_exp / denominator[:, :, None, None]).astype(jnp.float32)
        context_weights = rounded(context_exp / denominator[:, :, None]).astype(jnp.float32)
        return jnp.einsum('hqvk,vkhd->qhd', window_weights, value_band) + jnp.einsum('hqj,jhd->qhd', context_weights, context_values)
    attended = lax.map(row_step, jnp.arange(grid_rows, dtype=jnp.int32)).reshape(tokens, model_width)
    gated_heads = rounded(jax.nn.silu(silu_gate.astype(jnp.float32)) * attended)
    group_width = model_width // N_TP
    branch_sum = jnp.zeros((tokens, model_width), jnp.float32)
    for group_index in range(N_TP):
        first_col = group_index * group_width
        term = jnp.dot(gated_heads[:, first_col:first_col + group_width], w_out[first_col:first_col + group_width], preferred_element_type=jnp.float32)
        branch_sum = branch_sum + rounded(term).astype(jnp.float32)
    branch = rounded(branch_sum)
    updated = latent.astype(jnp.float32) + gating[0] * normalize(branch, gain_post)
    return updated.astype(jnp.bfloat16)
```

```python
import functools

import jax
import jax.numpy as jnp
from jax import lax
from jax.experimental import pallas as pl
from jax.experimental.pallas import tpu as pltpu
from jax.sharding import PartitionSpec as P

GRID_W = 64
WIN_ROWS = 8
WIN_COLS = 16
EPSILON = 1e-06
MASKED = -1e30
F32 = jnp.float32
BF16 = jnp.bfloat16
TILE = 256


def remote(src, dst, send, recv, where):
    return pltpu.make_async_remote_copy(
        src_ref=src,
        dst_ref=dst,
        send_sem=send,
        recv_sem=recv,
        device_id=where,
        device_id_type=pl.DeviceIdType.MESH,
    )


def dot(a, b):
    return jnp.dot(a, b, preferred_element_type=F32)


def dot_t(a, b):
    return lax.dot_general(a, b, (((1,), (1,)), ((), ())), preferred_element_type=F32)


def kernel(
    S,
    T,
    active,
    gain_pre,
    gain_post,
    table_rows,
    latent_hbm,
    context_hbm,
    wsh_hbm,
    wsc_hbm,
    wga_hbm,
    wq_hbm,
    wk_hbm,
    wv_hbm,
    ws_hbm,
    wo_hbm,
    out,
    lat,
    ctx,
    wmod,
    wall,
    wo,
    part,
    modbuf,
    modfull,
    modrow,
    norm_lat,
    norm_ctx,
    hid_lat,
    hid_ctx,
    qg,
    kv,
    ckv,
    table,
    gated,
    prod,
    terms,
    load_sem,
    a_send,
    a_recv,
    b_send,
    b_recv,
    y_send,
    y_recv,
    z_send,
    z_recv,
    h_send,
    h_recv,
    r_send,
    r_recv,
):
    s = lax.axis_index("sp")
    t = lax.axis_index("tp")
    tokens, width = lat.shape
    n_ctx = ctx.shape[0]
    cols = wo.shape[0]
    heads = table.shape[0]
    rows = tokens // GRID_W
    Y = max(1, T // 2)
    if S % Y:
        Y = 1
    Z = S // Y
    z = s // Y
    y = s % Y

    loads = []
    for i, (src, dst) in enumerate(
        [
            (wsh_hbm, wmod.at[0]),
            (wsc_hbm, wmod.at[1]),
            (wga_hbm, wmod.at[2]),
            (context_hbm, ctx),
            (latent_hbm, lat),
            (wk_hbm, wall.at[:, pl.ds(0, cols)]),
            (wv_hbm, wall.at[:, pl.ds(cols, cols)]),
            (wq_hbm, wall.at[:, pl.ds(2 * cols, cols)]),
            (ws_hbm, wall.at[:, pl.ds(3 * cols, cols)]),
            (wo_hbm, wo),
        ]
    ):
        copy = pltpu.make_async_copy(src, dst, load_sem.at[i])
        copy.start()
        loads.append(copy)

    barrier = pltpu.get_barrier_semaphore()
    for d in range(1, S):
        pl.semaphore_signal(
            barrier, inc=1, device_id={"sp": lax.rem(s + d, S)}, device_id_type=pl.DeviceIdType.MESH
        )
    for d in range(1, T):
        pl.semaphore_signal(
            barrier, inc=1, device_id={"tp": lax.rem(t + d, T)}, device_id_type=pl.DeviceIdType.MESH
        )

    part[...] = jnp.zeros_like(part)
    for i in range(3):
        loads[i].wait()
        part[2 * i : 2 * i + 2, :] = dot(active[...], wmod[i])[0:2]
    pl.semaphore_wait(barrier, S - 1 + T - 1)

    a_copies = []
    for d in range(1, S):
        copy = remote(
            part, modbuf.at[s], a_send.at[d - 1], a_recv.at[d - 1], {"sp": lax.rem(s + d, S)}
        )
        copy.start()
        a_copies.append(copy)

    def normalise(src, dst):
        step = 32

        @pl.loop(0, src.shape[0] // step)
        def _(i):
            at = pl.ds(pl.multiple_of(i * step, step), step)
            v = src[at, :].astype(F32)
            inv = lax.rsqrt(jnp.mean(v * v, axis=-1, keepdims=True) + EPSILON)
            dst[at, :] = v * inv * gain_pre[...]

    loads[3].wait()
    normalise(ctx, norm_ctx)
    loads[4].wait()

    modbuf[s] = part[...]
    for copy in a_copies:
        copy.wait()
    modfull[t] = jnp.sum(modbuf[...], axis=0)
    b_copies = []
    for d in range(1, T):
        copy = remote(
            modfull.at[t],
            modfull.at[t],
            b_send.at[d - 1],
            b_recv.at[d - 1],
            {"tp": lax.rem(t + d, T)},
        )
        copy.start()
        b_copies.append(copy)

    normalise(lat, norm_lat)

    for copy in b_copies:
        copy.wait()
    for j in range(T):
        modrow[:, j * cols : (j + 1) * cols] = modfull[j]

    def modulate(src, dst, shift, scale):
        step = 32

        @pl.loop(0, src.shape[0] // step)
        def _(i):
            at = pl.ds(pl.multiple_of(i * step, step), step)
            v = src[at, :] * (1.0 + modrow[scale : scale + 1, :]) + modrow[shift : shift + 1, :]
            dst[at, :] = v.astype(BF16)

    modulate(norm_ctx, hid_ctx, 1, 3)
    loads[5].wait()
    loads[6].wait()
    own_ctx = pl.ds(pl.multiple_of(s * n_ctx, n_ctx), n_ctx)

    @pl.loop(0, 2 * cols // TILE)
    def _(i):
        at = pl.ds(pl.multiple_of(i * TILE, TILE), TILE)
        ckv[own_ctx, at] = dot(hid_ctx[...], wall[:, at]).astype(BF16)

    y_copies = []
    for d in range(1, Y):
        copy = remote(
            ckv.at[own_ctx],
            ckv.at[own_ctx],
            y_send.at[d - 1],
            y_recv.at[d - 1],
            {"sp": z * Y + lax.rem(y + d, Y)},
        )
        copy.start()
        y_copies.append(copy)

    modulate(norm_lat, hid_lat, 0, 2)

    @pl.loop(0, 2 * cols // TILE)
    def _(i):
        at = pl.ds(pl.multiple_of(i * TILE, TILE), TILE)
        kv[tokens : 2 * tokens, at] = dot(hid_lat[...], wall[:, at]).astype(BF16)

    own_kv = kv.at[pl.ds(tokens, tokens)]
    to_next = remote(
        own_kv, kv.at[pl.ds(0, tokens)], h_send.at[0], h_recv.at[0], {"sp": lax.rem(s + 1, S)}
    )
    to_prev = remote(
        own_kv,
        kv.at[pl.ds(2 * tokens, tokens)],
        h_send.at[1],
        h_recv.at[1],
        {"sp": lax.rem(s + S - 1, S)},
    )

    for copy in y_copies:
        copy.wait()

    def block_of(k):
        size = Y * n_ctx
        return ckv.at[pl.ds(pl.multiple_of(k * size, size), size)]

    def up(k):
        return remote(
            block_of(z - k),
            block_of(z - k),
            z_send.at[0, k],
            z_recv.at[0, k],
            {"sp": lax.rem(s + Y, S)},
        )

    def down(k):
        return remote(
            block_of(z + k),
            block_of(z + k),
            z_send.at[1, k],
            z_recv.at[1, k],
            {"sp": lax.rem(s + S - Y, S)},
        )

    def send_up(k):
        return (z - k >= 0) & (z < Z - 1)

    def send_down(k):
        return (z + k <= Z - 1) & (z > 0)

    def z_start(k):
        @pl.when(send_up(k))
        def _():
            up(k).start()

        @pl.when(send_down(k))
        def _():
            down(k).start()

    def z_arrive(k):
        @pl.when(z - 1 - k >= 0)
        def _():
            b = block_of(z - 1 - k)
            remote(
                b, b, z_send.at[0, k], z_recv.at[0, k], {"sp": lax.rem(s + Y, S)}
            ).wait_recv()

        @pl.when(z + 1 + k <= Z - 1)
        def _():
            b = block_of(z + 1 + k)
            remote(
                b, b, z_send.at[1, k], z_recv.at[1, k], {"sp": lax.rem(s + S - Y, S)}
            ).wait_recv()

    if Z > 1:
        z_start(0)

    @pl.when(s < S - 1)
    def _():
        to_next.start()

    @pl.when(s > 0)
    def _():
        to_prev.start()

    loads[7].wait()
    loads[8].wait()

    @pl.loop(0, 2 * cols // TILE)
    def _(i):
        at = pl.ds(pl.multiple_of(i * TILE, TILE), TILE)
        wat = pl.ds(pl.multiple_of(2 * cols + i * TILE, TILE), TILE)
        qg[:, at] = dot(hid_lat[...], wall[:, wat]).astype(BF16)

    lane = lax.broadcasted_iota(jnp.int32, (GRID_W, 2 * GRID_W), 1) % GRID_W
    row = lax.broadcasted_iota(jnp.int32, (GRID_W, 2 * GRID_W), 0)
    first = jnp.clip(row - WIN_COLS // 2, 0, GRID_W - WIN_COLS)
    inside = (lane >= first) & (lane < first + WIN_COLS)
    pairs = table.shape[1]

    @pl.loop(0, heads)
    def _(h):
        for p in range(pairs):
            line = jnp.broadcast_to(table_rows[h, p : p + 1, :], (GRID_W, 2 * GRID_W))
            rolled = pltpu.roll(
                line, 2 * GRID_W - (WIN_COLS - 1), 1, stride=1, stride_axis=0
            )
            table[h, p] = jnp.where(inside, rolled, MASKED)

    for k in range(Z - 1):
        z_arrive(k)
        if k + 1 < Z - 1:
            z_start(k + 1)

    @pl.when(s > 0)
    def _():
        to_next.wait_recv()

    @pl.when(s < S - 1)
    def _():
        to_prev.wait_recv()

    total_rows = rows * S
    half = lax.broadcasted_iota(jnp.int32, (tokens, 128), 1) < 64
    scale = 0.125

    @pl.loop(0, heads // 2)
    def _(hp):
        at = pl.ds(pl.multiple_of(hp * 128, 128), 128)
        vat = pl.ds(pl.multiple_of(cols + hp * 128, 128), 128)
        q2 = qg[:, at].astype(F32) * scale
        ck = ckv[:, at]
        cv = ckv[:, vat]
        outs = []
        for e in range(2):
            q = jnp.where(half if e == 0 else jnp.logical_not(half), q2, 0.0).astype(BF16)
            sc = dot_t(q, ck)
            sw = []
            bands = []
            for r in range(rows):
                g = s * rows + r
                rs = jnp.clip(g - WIN_ROWS // 2, 0, total_rows - WIN_ROWS)
                band = pl.ds(
                    pl.multiple_of((rs - s * rows + rows) * GRID_W, GRID_W), WIN_ROWS * GRID_W
                )
                bands.append(band)
                bias = jnp.concatenate(
                    [
                        table[hp * 2 + e, rs - g + WIN_ROWS - 1 + 2 * p]
                        for p in range(WIN_ROWS // 2)
                    ],
                    axis=1,
                )
                sw.append(dot_t(q[r * GRID_W : (r + 1) * GRID_W], kv[band, at]) + bias)
            sw = jnp.concatenate(sw, axis=0)
            m = jnp.maximum(
                jnp.max(sc, axis=-1, keepdims=True), jnp.max(sw, axis=-1, keepdims=True)
            )
            pc = jnp.exp(sc - m)
            pw = jnp.exp(sw - m)
            total = jnp.sum(pc, axis=-1, keepdims=True) + jnp.sum(pw, axis=-1, keepdims=True)
            pw = pw.astype(BF16)
            o = dot(pc.astype(BF16), cv)
            ow = [
                dot(pw[r * GRID_W : (r + 1) * GRID_W], kv[bands[r], vat]) for r in range(rows)
            ]
            outs.append((o + jnp.concatenate(ow, axis=0)) / total)
        o = jnp.where(half, outs[0], outs[1])
        gate = qg[:, vat].astype(F32)
        gated[:, at] = (gate / (1.0 + jnp.exp(-gate)) * o).astype(BF16)

    loads[9].wait()
    own = tokens // T

    @pl.loop(0, width // TILE)
    def _(i):
        at = pl.ds(pl.multiple_of(i * TILE, TILE), TILE)
        prod[:, at] = dot(gated[...], wo[:, at]).astype(BF16)

    r_copies = []
    for d in range(1, T):
        other = lax.rem(t + d, T)
        copy = remote(
            prod.at[pl.ds(pl.multiple_of(other * own, own), own)],
            terms.at[d - 1],
            r_send.at[d - 1],
            r_recv.at[d - 1],
            {"tp": other},
        )
        copy.start()
        r_copies.append(copy)

    own_at = pl.ds(pl.multiple_of(t * own, own), own)
    total = prod[own_at, :].astype(F32)
    for i, copy in enumerate(r_copies):
        copy.wait()
        total = total + terms[i].astype(F32)
    b = total.astype(BF16).astype(F32)
    inv = lax.rsqrt(jnp.mean(b * b, axis=-1, keepdims=True) + EPSILON)
    out[...] = (
        lat[own_at, :].astype(F32) + modrow[4:5, :] * (b * inv * gain_post[...])
    ).astype(BF16)

    for k in range(Z - 1):

        @pl.when(send_up(k))
        def _():
            up(k).wait_send()

        @pl.when(send_down(k))
        def _():
            down(k).wait_send()

    @pl.when(s < S - 1)
    def _():
        to_next.wait_send()

    @pl.when(s > 0)
    def _():
        to_prev.wait_send()


def shards(
    S,
    T,
    latent,
    context,
    condition,
    context_condition,
    gain_pre,
    gain_post,
    w_shift,
    w_scale,
    w_gate,
    w_query,
    w_key,
    w_value,
    w_silu,
    offset_bias,
    w_out,
):
    in_rows, cols = w_shift.shape
    tokens, width = latent.shape
    n_ctx = context.shape[0]
    heads = offset_bias.shape[0]
    stacked = jnp.stack([condition, context_condition])
    own = lax.dynamic_slice_in_dim(stacked, lax.axis_index("sp") * in_rows, in_rows, 1)
    active = jnp.pad(jax.nn.silu(own.astype(F32)).astype(BF16), ((0, 14), (0, 0)))
    wide = jnp.pad(offset_bias, ((0, 0), (0, 0), (0, GRID_W - offset_bias.shape[2])))
    table_rows = jnp.concatenate([wide[:, :-1], wide[:, 1:]], axis=-1)
    pairs = table_rows.shape[1]
    own_rows = tokens // T
    vmem = pl.BlockSpec(memory_space=pltpu.VMEM)
    hbm = pl.BlockSpec(memory_space=pl.ANY)
    sem = pltpu.SemaphoreType.DMA
    Y = max(1, T // 2)
    if S % Y:
        Y = 1
    Z = S // Y
    return pl.pallas_call(
        functools.partial(kernel, S, T),
        out_shape=jax.ShapeDtypeStruct((own_rows, width), BF16),
        in_specs=[vmem] * 4 + [hbm] * 10,
        out_specs=vmem,
        scratch_shapes=[
            pltpu.VMEM((tokens, width), BF16),
            pltpu.VMEM((n_ctx, width), BF16),
            pltpu.VMEM((3, in_rows, cols), BF16),
            pltpu.VMEM((width, 4 * cols), BF16),
            pltpu.VMEM((cols, width), BF16),
            pltpu.VMEM((8, cols), F32),
            pltpu.VMEM((S, 8, cols), F32),
            pltpu.VMEM((T, 8, cols), F32),
            pltpu.VMEM((8, width), F32),
            pltpu.VMEM((tokens, width), F32),
            pltpu.VMEM((n_ctx, width), F32),
            pltpu.VMEM((tokens, width), BF16),
            pltpu.VMEM((n_ctx, width), BF16),
            pltpu.VMEM((tokens, 2 * cols), BF16),
            pltpu.VMEM((3 * tokens, 2 * cols), BF16),
            pltpu.VMEM((S * n_ctx, 2 * cols), BF16),
            pltpu.VMEM((heads, pairs, GRID_W, 2 * GRID_W), F32),
            pltpu.VMEM((tokens, cols), BF16),
            pltpu.VMEM((tokens, width), BF16),
            pltpu.VMEM((max(T - 1, 1), own_rows, width), BF16),
            sem((10,)),
            sem((max(S - 1, 1),)),
            sem((max(S - 1, 1),)),
            sem((max(T - 1, 1),)),
            sem((max(T - 1, 1),)),
            sem((max(Y - 1, 1),)),
            sem((max(Y - 1, 1),)),
            sem((2, max(Z - 1, 1))),
            sem((2, max(Z - 1, 1))),
            sem((2,)),
            sem((2,)),
            sem((max(T - 1, 1),)),
            sem((max(T - 1, 1),)),
        ],
        compiler_params=pltpu.CompilerParams(
            collective_id=0, has_side_effects=True, vmem_limit_bytes=60 * 1024 * 1024
        ),
    )(
        active,
        gain_pre.reshape(1, width),
        gain_post.reshape(1, width),
        table_rows,
        latent,
        context,
        w_shift,
        w_scale,
        w_gate,
        w_query,
        w_key,
        w_value,
        w_silu,
        w_out,
    )


def solution(mesh):
    in_specs = (
        P("sp", None),
        P("sp", None),
        P(),
        P(),
        P(),
        P(),
        P("sp", "tp"),
        P("sp", "tp"),
        P("sp", "tp"),
        P(None, "tp"),
        P(None, "tp"),
        P(None, "tp"),
        P(None, "tp"),
        P("tp", None, None),
        P("tp", None),
    )
    return jax.shard_map(
        functools.partial(shards, mesh.shape["sp"], mesh.shape["tp"]),
        mesh=mesh,
        in_specs=in_specs,
        out_specs=P(("sp", "tp"), None),
        check_vma=False,
    )
```

```python
import functools

import jax
import jax.numpy as jnp
from jax import lax
from jax.experimental import pallas as pl
from jax.experimental.pallas import tpu as pltpu
from jax.sharding import PartitionSpec as P

GRID_W = 64
WIN_ROWS = 8
WIN_COLS = 16
EPSILON = 1e-06
MASKED = -1e30
F32 = jnp.float32
BF16 = jnp.bfloat16
TILE = 256


def remote(src, dst, send, recv, where):
    return pltpu.make_async_remote_copy(
        src_ref=src,
        dst_ref=dst,
        send_sem=send,
        recv_sem=recv,
        device_id=where,
        device_id_type=pl.DeviceIdType.MESH,
    )


def dot(a, b):
    return jnp.dot(a, b, preferred_element_type=F32)


def dot_t(a, b):
    return lax.dot_general(a, b, (((1,), (1,)), ((), ())), preferred_element_type=F32)


def kernel(
    S,
    T,
    active,
    gain_pre,
    gain_post,
    table_rows,
    latent_hbm,
    context_hbm,
    wsh_hbm,
    wsc_hbm,
    wga_hbm,
    wq_hbm,
    wk_hbm,
    wv_hbm,
    ws_hbm,
    wo_hbm,
    out,
    lat,
    ctx,
    wmod,
    wall,
    wo,
    part,
    modbuf,
    modfull,
    modrow,
    hid,
    qg,
    kv,
    ckv,
    table,
    gated,
    prod,
    pair,
    mate,
    terms,
    load_sem,
    a_send,
    a_recv,
    b_send,
    b_recv,
    y_send,
    y_recv,
    z_send,
    z_recv,
    x_send,
    x_recv,
    d_send,
    d_recv,
    h_send,
    h_recv,
    m_send,
    m_recv,
    r_send,
    r_recv,
):
    s = lax.axis_index("sp")
    t = lax.axis_index("tp")
    width = lat.shape[1]
    tokens = lat.shape[0] // 3
    n_ctx = ctx.shape[0] // S
    cols = wo.shape[0]
    heads = table.shape[0]
    rows = tokens // GRID_W
    X, Y, Z = layout_of(S, T)
    z = s // Y
    y = s % Y
    xi = t // 2
    core = t % 2
    partner = {"tp": t + 1 - 2 * core}
    half_width = width // 2
    slice_width = width // T
    own_lat = pl.ds(tokens, tokens)

    def ctx_rows(b):
        return pl.ds(pl.multiple_of(b * n_ctx, n_ctx), n_ctx)

    def ctx_slice(b, j):
        return ctx.at[ctx_rows(b), pl.ds(pl.multiple_of(j * slice_width, slice_width), slice_width)]

    loads = []
    for i, (src, dst) in enumerate(
        [
            (context_hbm, ctx.at[ctx_rows(s)]),
            (wsh_hbm, wmod.at[0]),
            (wsc_hbm, wmod.at[1]),
            (wga_hbm, wmod.at[2]),
            (latent_hbm, lat.at[own_lat]),
            (wk_hbm, wall.at[:, pl.ds(0, cols)]),
            (wv_hbm, wall.at[:, pl.ds(cols, cols)]),
            (wq_hbm, wall.at[:, pl.ds(2 * cols, cols)]),
            (ws_hbm, wall.at[:, pl.ds(3 * cols, cols)]),
            (wo_hbm, wo),
        ]
    ):
        copy = pltpu.make_async_copy(src, dst, load_sem.at[i])
        copy.start()
        loads.append(copy)

    barrier = pltpu.get_barrier_semaphore()
    for d in range(1, S):
        pl.semaphore_signal(
            barrier, inc=1, device_id={"sp": lax.rem(s + d, S)}, device_id_type=pl.DeviceIdType.MESH
        )
    for d in range(1, T):
        pl.semaphore_signal(
            barrier, inc=1, device_id={"tp": lax.rem(t + d, T)}, device_id_type=pl.DeviceIdType.MESH
        )

    pending = []

    def send(cond, copy):
        pending.append((cond, copy))
        if cond is None:
            copy.start()
        else:

            @pl.when(cond)
            def _():
                copy.start()

    def arrive(cond, copy):
        if cond is None:
            copy.wait_recv()
        else:

            @pl.when(cond)
            def _():
                copy.wait_recv()

    part[...] = jnp.zeros_like(part)
    loads[0].wait()
    pl.semaphore_wait(barrier, S - 1 + T - 1)

    for d in range(1, Y):
        send(
            None,
            remote(
                ctx_slice(s, t),
                ctx_slice(s, t),
                y_send.at[d - 1],
                y_recv.at[d - 1],
                {"sp": z * Y + lax.rem(y + d, Y)},
            ),
        )

    for i in range(3):
        loads[1 + i].wait()
        part[2 * i : 2 * i + 2, :] = dot(active[...], wmod[i])[0:2]

    a_copies = []
    for d in range(1, S):
        copy = remote(
            part, modbuf.at[s], a_send.at[d - 1], a_recv.at[d - 1], {"sp": lax.rem(s + d, S)}
        )
        copy.start()
        a_copies.append(copy)

    loads[4].wait()

    def lat_part(where, side):
        return lat.at[
            pl.ds(where * tokens, tokens),
            pl.ds(pl.multiple_of(side * half_width, half_width), half_width),
        ]

    to_next = remote(
        lat_part(1, core), lat_part(0, core), h_send.at[0], h_recv.at[0], {"sp": lax.rem(s + 1, S)}
    )
    to_prev = remote(
        lat_part(1, core),
        lat_part(2, core),
        h_send.at[1],
        h_recv.at[1],
        {"sp": lax.rem(s + S - 1, S)},
    )
    send(s < S - 1, to_next)
    send(s > 0, to_prev)

    def units_of(k):
        if k < 0:
            return [(d - 1, z * Y + lax.rem(y + Y - d, Y), None) for d in range(1, Y)]
        units = []
        for way in range(2):
            at = z - 1 - k if way == 0 else z + 1 + k
            have = at >= 0 if way == 0 else at <= Z - 1
            for u in range(Y):
                units.append((Y - 1 + (k * 2 + way) * Y + u, at * Y + u, have))
        return units

    def chain(way, k, u):
        at = z - k if way == 0 else z + k
        have = ((at >= 0) & (z < Z - 1)) if way == 0 else ((at <= Z - 1) & (z > 0))
        target = lax.rem(s + Y, S) if way == 0 else lax.rem(s + S - Y, S)
        b = ctx_slice(at * Y + u, t)
        return have, remote(b, b, z_send.at[way, k, u], z_recv.at[way, k, u], {"sp": target})

    def chain_start(k):
        if k < Z - 1:
            for u in range(Y):
                for way in range(2):
                    send(*chain(way, k, u))

    def share(unit):
        n, b, have = unit
        mine = ctx_slice(b, t)
        for d in range(1, X):
            send(
                have,
                remote(
                    mine,
                    mine,
                    x_send.at[n * (X - 1) + d - 1] if X > 1 else None,
                    x_recv.at[n * (X - 1) + d - 1] if X > 1 else None,
                    {"tp": lax.rem(xi + d, X) * 2 + core},
                ),
            )
        send(have, remote(mine, mine, d_send.at[n * X], d_recv.at[n * X], partner))

    def own_arrive(k):
        if k < 0:
            for d in range(1, Y):
                b = ctx_slice(z * Y + lax.rem(y + Y - d, Y), t)
                arrive(None, remote(b, b, y_send.at[d - 1], y_recv.at[d - 1], partner))
        else:
            for n, b, have in units_of(k):
                way, u = ((n - (Y - 1)) // Y) % 2, (n - (Y - 1)) % Y
                ref = ctx_slice(b, t)
                arrive(
                    have,
                    remote(ref, ref, z_send.at[way, k, u], z_recv.at[way, k, u], partner),
                )
        chain_start(k + 1)
        for unit in units_of(k):
            share(unit)

    def x_arrive(k):
        for n, b, have in units_of(k):
            for d in range(1, X):
                ref = ctx_slice(b, lax.rem(xi + X - d, X) * 2 + core)
                at = n * (X - 1) + d - 1
                arrive(have, remote(ref, ref, x_send.at[at], x_recv.at[at], partner))
                send(
                    have, remote(ref, ref, d_send.at[n * X + d], d_recv.at[n * X + d], partner)
                )

    def mate_arrive(k):
        for n, b, have in units_of(k):
            for d in range(X):
                ref = ctx_slice(b, lax.rem(xi + X - d, X) * 2 + 1 - core)
                arrive(have, remote(ref, ref, d_send.at[n * X + d], d_recv.at[n * X + d], partner))

    def hidden(src, first, count, kind):
        step = 32

        @pl.loop(0, count // step)
        def _(i):
            at = pl.ds(pl.multiple_of(first + i * step, step), step)
            v = src[at, :].astype(F32)
            inv = lax.rsqrt(jnp.mean(v * v, axis=-1, keepdims=True) + EPSILON)
            v = v * inv * modrow[2 + kind : 3 + kind, :] + modrow[kind : kind + 1, :]
            hid[pl.ds(pl.multiple_of(i * step, step), step), :] = v.astype(BF16)

    def project(count, dst, first, tiles, start):
        @pl.loop(0, tiles)
        def _(i):
            at = pl.ds(pl.multiple_of(i * TILE, TILE), TILE)
            wat = pl.ds(pl.multiple_of(start + i * TILE, TILE), TILE)
            dst[pl.ds(first, count), at] = dot(hid[0:count, :], wall[:, wat]).astype(BF16)

    def ctx_project(at):
        count = Y * n_ctx
        first = pl.multiple_of(at * count, count)
        hidden(ctx, first, count, 1)
        project(count, ckv, first, 2 * cols // TILE, 0)

    def process(k):
        mate_arrive(k)
        if k < 0:
            ctx_project(z)
        else:

            @pl.when(z - 1 - k >= 0)
            def _():
                ctx_project(z - 1 - k)

            @pl.when(z + 1 + k <= Z - 1)
            def _():
                ctx_project(z + 1 + k)

    own_arrive(-1)

    lane = lax.broadcasted_iota(jnp.int32, (GRID_W, 2 * GRID_W), 1) % GRID_W
    row = lax.broadcasted_iota(jnp.int32, (GRID_W, 2 * GRID_W), 0)
    first = jnp.clip(row - WIN_COLS // 2, 0, GRID_W - WIN_COLS)
    inside = (lane >= first) & (lane < first + WIN_COLS)
    pairs = table.shape[1]

    @pl.loop(0, heads)
    def _(h):
        for p in range(pairs):
            line = jnp.broadcast_to(table_rows[h, p : p + 1, :], (GRID_W, 2 * GRID_W))
            rolled = pltpu.roll(
                line, 2 * GRID_W - (WIN_COLS - 1), 1, stride=1, stride_axis=0
            )
            table[h, p] = jnp.where(inside, rolled, MASKED)

    modbuf[s] = part[...]
    for copy in a_copies:
        copy.wait()
    modfull[t] = jnp.sum(modbuf[...], axis=0)
    b_copies = []
    for d in range(1, T):
        copy = remote(
            modfull.at[t],
            modfull.at[t],
            b_send.at[d - 1],
            b_recv.at[d - 1],
            {"tp": lax.rem(t + d, T)},
        )
        copy.start()
        b_copies.append(copy)

    x_arrive(-1)
    if Z > 1:
        own_arrive(0)
    for copy in b_copies:
        copy.wait()
    for j in range(T):
        at = slice(j * cols, (j + 1) * cols)
        modrow[:, at] = modfull[j]
        modrow[2:4, at] = gain_pre[:, at] * (1.0 + modfull[j, 2:4])

    for i in range(5, 9):
        loads[i].wait()
    hidden(lat, tokens, tokens, 0)
    project(tokens, kv, tokens, 2 * cols // TILE, 0)
    project(tokens, qg, 0, 2 * cols // TILE, 2 * cols)

    def halo_share():
        arrive(s > 0, to_next)
        send(
            s > 0,
            remote(lat_part(0, core), lat_part(0, core), m_send.at[0], m_recv.at[0], partner),
        )
        arrive(s < S - 1, to_prev)
        send(
            s < S - 1,
            remote(lat_part(2, core), lat_part(2, core), m_send.at[1], m_recv.at[1], partner),
        )

    for k in range(1, Z - 1):
        own_arrive(k)
        x_arrive(k - 1)
        process(k - 2)
    if Z > 1:
        x_arrive(Z - 2)
        if Z > 2:
            process(Z - 3)
    halo_share()
    if Z > 1:
        process(Z - 2)
    else:
        process(-1)

    @pl.when(s > 0)
    def _():
        ref = lat_part(0, 1 - core)
        remote(ref, ref, m_send.at[0], m_recv.at[0], partner).wait_recv()
        hidden(lat, 0, tokens, 0)
        project(tokens, kv, 0, 2 * cols // TILE, 0)

    @pl.when(s < S - 1)
    def _():
        ref = lat_part(2, 1 - core)
        remote(ref, ref, m_send.at[1], m_recv.at[1], partner).wait_recv()
        hidden(lat, 2 * tokens, tokens, 0)
        project(tokens, kv, 2 * tokens, 2 * cols // TILE, 0)

    total_rows = rows * S
    half = lax.broadcasted_iota(jnp.int32, (tokens, 128), 1) < 64
    scale = 0.125

    @pl.loop(0, heads // 2)
    def _(hp):
        at = pl.ds(pl.multiple_of(hp * 128, 128), 128)
        vat = pl.ds(pl.multiple_of(cols + hp * 128, 128), 128)
        q2 = qg[:, at].astype(F32) * scale
        ck = ckv[:, at]
        cv = ckv[:, vat]
        outs = []
        for e in range(2):
            q = jnp.where(half if e == 0 else jnp.logical_not(half), q2, 0.0).astype(BF16)
            sc = dot_t(q, ck)
            sw = []
            bands = []
            for r in range(rows):
                g = s * rows + r
                rs = jnp.clip(g - WIN_ROWS // 2, 0, total_rows - WIN_ROWS)
                band = pl.ds(
                    pl.multiple_of((rs - s * rows + rows) * GRID_W, GRID_W), WIN_ROWS * GRID_W
                )
                bands.append(band)
                bias = jnp.concatenate(
                    [
                        table[hp * 2 + e, rs - g + WIN_ROWS - 1 + 2 * p]
                        for p in range(WIN_ROWS // 2)
                    ],
                    axis=1,
                )
                sw.append(dot_t(q[r * GRID_W : (r + 1) * GRID_W], kv[band, at]) + bias)
            sw = jnp.concatenate(sw, axis=0)
            m = jnp.maximum(
                jnp.max(sc, axis=-1, keepdims=True), jnp.max(sw, axis=-1, keepdims=True)
            )
            pc = jnp.exp(sc - m)
            pw = jnp.exp(sw - m)
            total = jnp.sum(pc, axis=-1, keepdims=True) + jnp.sum(pw, axis=-1, keepdims=True)
            pw = pw.astype(BF16)
            o = dot(pc.astype(BF16), cv)
            ow = [
                dot(pw[r * GRID_W : (r + 1) * GRID_W], kv[bands[r], vat]) for r in range(rows)
            ]
            outs.append((o + jnp.concatenate(ow, axis=0)) / total)
        o = jnp.where(half, outs[0], outs[1])
        gate = qg[:, vat].astype(F32)
        gated[:, at] = (gate / (1.0 + jnp.exp(-gate)) * o).astype(BF16)

    loads[9].wait()
    own = tokens // T
    groups = 4
    span = width // groups
    m_copies = []
    for g in range(groups):
        span_at = pl.ds(g * span, span)
        prod[:, span_at] = dot(gated[...], wo[:, span_at]).astype(BF16)
        copies = []
        for i in range(X):
            n = g * X + i
            copy = remote(
                prod.at[
                    pl.ds(pl.multiple_of((i * 2 + 1 - core) * own, own), own), span_at
                ],
                mate.at[i, :, span_at],
                m_send.at[2 + n],
                m_recv.at[2 + n],
                partner,
            )
            copy.start()
            copies.append(copy)
        m_copies.append(copies)
    r_copies = []
    for g in range(groups):
        span_at = pl.ds(g * span, span)
        for copy in m_copies[g]:
            copy.wait()
        copies = []
        for i in range(X):
            at = pl.ds(pl.multiple_of((i * 2 + core) * own, own), own)
            pair[i, :, span_at] = (
                prod[at, span_at].astype(F32) + mate[i, :, span_at].astype(F32)
            )
            if X > 1:
                prod[at, span_at] = pair[i, :, span_at].astype(BF16)
        for d in range(1, X):
            other = lax.rem(xi + d, X)
            n = g * (X - 1) + d - 1
            copy = remote(
                prod.at[pl.ds(pl.multiple_of((other * 2 + core) * own, own), own), span_at],
                terms.at[d - 1, :, span_at],
                r_send.at[n],
                r_recv.at[n],
                {"tp": other * 2 + core},
            )
            copy.start()
            copies.append(copy)
        r_copies.append(copies)
    for copies in r_copies:
        for copy in copies:
            copy.wait()
    total = pair[xi]
    for d in range(1, X):
        total = total + terms[d - 1].astype(F32)
    b = total.astype(BF16).astype(F32)
    inv = lax.rsqrt(jnp.mean(b * b, axis=-1, keepdims=True) + EPSILON)
    own_at = pl.ds(pl.multiple_of(tokens + t * own, own), own)
    out[...] = (
        lat[own_at, :].astype(F32) + modrow[4:5, :] * (b * inv * gain_post[...])
    ).astype(BF16)

    for cond, copy in pending:
        if cond is None:
            copy.wait_send()
        else:

            @pl.when(cond)
            def _(copy=copy):
                copy.wait_send()


def layout_of(S, T):
    X = T // 2
    Y = X if S % X == 0 else 1
    return X, Y, S // Y


def shards(
    S,
    T,
    latent,
    context,
    condition,
    context_condition,
    gain_pre,
    gain_post,
    w_shift,
    w_scale,
    w_gate,
    w_query,
    w_key,
    w_value,
    w_silu,
    offset_bias,
    w_out,
):
    in_rows, cols = w_shift.shape
    tokens, width = latent.shape
    n_ctx = context.shape[0]
    heads = offset_bias.shape[0]
    stacked = jnp.stack([condition, context_condition])
    own = lax.dynamic_slice_in_dim(stacked, lax.axis_index("sp") * in_rows, in_rows, 1)
    active = jnp.pad(jax.nn.silu(own.astype(F32)).astype(BF16), ((0, 14), (0, 0)))
    wide = jnp.pad(offset_bias, ((0, 0), (0, 0), (0, GRID_W - offset_bias.shape[2])))
    table_rows = jnp.concatenate([wide[:, :-1], wide[:, 1:]], axis=-1)
    pairs = table_rows.shape[1]
    own_rows = tokens // T
    vmem = pl.BlockSpec(memory_space=pltpu.VMEM)
    hbm = pl.BlockSpec(memory_space=pl.ANY)
    sem = pltpu.SemaphoreType.DMA
    X, Y, Z = layout_of(S, T)
    units = Y - 1 + 2 * (Z - 1) * Y
    return pl.pallas_call(
        functools.partial(kernel, S, T),
        out_shape=jax.ShapeDtypeStruct((own_rows, width), BF16),
        in_specs=[vmem] * 4 + [hbm] * 10,
        out_specs=vmem,
        scratch_shapes=[
            pltpu.VMEM((3 * tokens, width), BF16),
            pltpu.VMEM((S * n_ctx, width), BF16),
            pltpu.VMEM((3, in_rows, cols), BF16),
            pltpu.VMEM((width, 4 * cols), BF16),
            pltpu.VMEM((cols, width), BF16),
            pltpu.VMEM((8, cols), F32),
            pltpu.VMEM((S, 8, cols), F32),
            pltpu.VMEM((T, 8, cols), F32),
            pltpu.VMEM((8, width), F32),
            pltpu.VMEM((max(tokens, Y * n_ctx), width), BF16),
            pltpu.VMEM((tokens, 2 * cols), BF16),
            pltpu.VMEM((3 * tokens, 2 * cols), BF16),
            pltpu.VMEM((S * n_ctx, 2 * cols), BF16),
            pltpu.VMEM((heads, pairs, GRID_W, 2 * GRID_W), F32),
            pltpu.VMEM((tokens, cols), BF16),
            pltpu.VMEM((tokens, width), BF16),
            pltpu.VMEM((X, own_rows, width), F32),
            pltpu.VMEM((X, own_rows, width), BF16),
            pltpu.VMEM((max(X - 1, 1), own_rows, width), BF16),
            sem((10,)),
            sem((max(S - 1, 1),)),
            sem((max(S - 1, 1),)),
            sem((max(T - 1, 1),)),
            sem((max(T - 1, 1),)),
            sem((max(Y - 1, 1),)),
            sem((max(Y - 1, 1),)),
            sem((2, max(Z - 1, 1), Y)),
            sem((2, max(Z - 1, 1), Y)),
            sem((max(units * (X - 1), 1),)),
            sem((max(units * (X - 1), 1),)),
            sem((max(units * X, 1),)),
            sem((max(units * X, 1),)),
            sem((2,)),
            sem((2,)),
            sem((2 + 4 * X,)),
            sem((2 + 4 * X,)),
            sem((4 * max(X - 1, 1),)),
            sem((4 * max(X - 1, 1),)),
        ],
        compiler_params=pltpu.CompilerParams(
            collective_id=0, has_side_effects=True, vmem_limit_bytes=60 * 1024 * 1024
        ),
    )(
        active,
        gain_pre.reshape(1, width),
        gain_post.reshape(1, width),
        table_rows,
        latent,
        context,
        w_shift,
        w_scale,
        w_gate,
        w_query,
        w_key,
        w_value,
        w_silu,
        w_out,
    )


def solution(mesh):
    in_specs = (
        P("sp", None),
        P("sp", None),
        P(),
        P(),
        P(),
        P(),
        P("sp", "tp"),
        P("sp", "tp"),
        P("sp", "tp"),
        P(None, "tp"),
        P(None, "tp"),
        P(None, "tp"),
        P(None, "tp"),
        P("tp", None, None),
        P("tp", None),
    )
    return jax.shard_map(
        functools.partial(shards, mesh.shape["sp"], mesh.shape["tp"]),
        mesh=mesh,
        in_specs=in_specs,
        out_specs=P(("sp", "tp"), None),
        check_vma=False,
    )
```

```python
import functools

import jax
import jax.numpy as jnp
from jax import lax
from jax.experimental import pallas as pl
from jax.experimental.pallas import tpu as pltpu
from jax.sharding import PartitionSpec as P

GRID_W = 64
WIN_ROWS = 8
WIN_COLS = 16
EPSILON = 1e-06
MASKED = -1e30
F32 = jnp.float32
BF16 = jnp.bfloat16
TILE = 512
PIECES = 4


def remote(src, dst, send, recv, where):
    return pltpu.make_async_remote_copy(
        src_ref=src,
        dst_ref=dst,
        send_sem=send,
        recv_sem=recv,
        device_id=where,
        device_id_type=pl.DeviceIdType.MESH,
    )


def dot(a, b):
    return jnp.dot(a, b, preferred_element_type=F32)


def dot_t(a, b):
    return lax.dot_general(a, b, (((1,), (1,)), ((), ())), preferred_element_type=F32)


def kernel(
    S,
    T,
    active,
    gain_pre,
    gain_post,
    table_rows,
    latent_hbm,
    context_hbm,
    wsh_hbm,
    wsc_hbm,
    wga_hbm,
    wq_hbm,
    wk_hbm,
    wv_hbm,
    ws_hbm,
    wo_hbm,
    out,
    lat,
    ctx,
    wmod,
    wall,
    wo,
    part,
    modbuf,
    modfull,
    modrow,
    hid,
    qg,
    kv,
    ckv,
    table,
    gated,
    prod,
    pair,
    mate,
    terms,
    load_sem,
    a_send,
    a_recv,
    b_send,
    b_recv,
    y_send,
    y_recv,
    z_send,
    z_recv,
    x_send,
    x_recv,
    d_send,
    d_recv,
    h_send,
    h_recv,
    m_send,
    m_recv,
    r_send,
    r_recv,
):
    s = lax.axis_index("sp")
    t = lax.axis_index("tp")
    width = lat.shape[1]
    tokens = lat.shape[0] // 3
    n_ctx = ctx.shape[0] // S
    cols = wo.shape[0]
    heads = table.shape[0]
    rows = tokens // GRID_W
    X, Y, Z = layout_of(S, T)
    z = s // Y
    y = s % Y
    xi = t // 2
    core = t % 2
    partner = {"tp": t + 1 - 2 * core}
    half_width = width // 2
    slice_width = width // T
    own_lat = pl.ds(tokens, tokens)

    def ctx_rows(b):
        return pl.ds(pl.multiple_of(b * n_ctx, n_ctx), n_ctx)

    def ctx_slice(b, j):
        return ctx.at[ctx_rows(b), pl.ds(pl.multiple_of(j * slice_width, slice_width), slice_width)]

    loads = []
    for i, (src, dst) in enumerate(
        [
            (context_hbm, ctx.at[ctx_rows(s)]),
            (wsh_hbm, wmod.at[0]),
            (wsc_hbm, wmod.at[1]),
            (wga_hbm, wmod.at[2]),
            (latent_hbm, lat.at[own_lat]),
            (wk_hbm, wall.at[:, pl.ds(0, cols)]),
            (wv_hbm, wall.at[:, pl.ds(cols, cols)]),
            (wq_hbm, wall.at[:, pl.ds(2 * cols, cols)]),
            (ws_hbm, wall.at[:, pl.ds(3 * cols, cols)]),
            (wo_hbm, wo),
        ]
    ):
        copy = pltpu.make_async_copy(src, dst, load_sem.at[i])
        copy.start()
        loads.append(copy)

    barrier = pltpu.get_barrier_semaphore()
    for d in range(1, S):
        pl.semaphore_signal(
            barrier, inc=1, device_id={"sp": lax.rem(s + d, S)}, device_id_type=pl.DeviceIdType.MESH
        )
    for d in range(1, T):
        pl.semaphore_signal(
            barrier, inc=1, device_id={"tp": lax.rem(t + d, T)}, device_id_type=pl.DeviceIdType.MESH
        )

    pending = []

    def send(cond, copy):
        pending.append((cond, copy))
        if cond is None:
            copy.start()
        else:

            @pl.when(cond)
            def _():
                copy.start()

    def arrive(cond, copy):
        if cond is None:
            copy.wait_recv()
        else:

            @pl.when(cond)
            def _():
                copy.wait_recv()

    part[...] = jnp.zeros_like(part)
    loads[0].wait()
    pl.semaphore_wait(barrier, S - 1 + T - 1)

    for d in range(1, Y):
        send(
            None,
            remote(
                ctx_slice(s, t),
                ctx_slice(s, t),
                y_send.at[d - 1],
                y_recv.at[d - 1],
                {"sp": z * Y + lax.rem(y + d, Y)},
            ),
        )

    def chain(way, k, u):
        at = z - k if way == 0 else z + k
        have = ((at >= 0) & (z < Z - 1)) if way == 0 else ((at <= Z - 1) & (z > 0))
        target = lax.rem(s + Y, S) if way == 0 else lax.rem(s + S - Y, S)
        b = ctx_slice(at * Y + lax.rem(y + u, Y), t)
        return have, remote(b, b, z_send.at[way, k, u], z_recv.at[way, k, u], {"sp": target})

    for way in range(2):
        if Z > 1:
            send(*chain(way, 0, 0))

    for i in range(3):
        loads[1 + i].wait()
        part[2 * i : 2 * i + 2, :] = dot(active[...], wmod[i])[0:2]

    a_copies = []
    for d in range(1, S):
        copy = remote(
            part, modbuf.at[s], a_send.at[d - 1], a_recv.at[d - 1], {"sp": lax.rem(s + d, S)}
        )
        copy.start()
        a_copies.append(copy)

    loads[4].wait()

    piece = half_width // PIECES

    def lat_part(where, side, p):
        return lat.at[
            pl.ds(where * tokens, tokens),
            pl.ds(pl.multiple_of(side * half_width + p * piece, piece), piece),
        ]

    def to_next(p):
        return remote(
            lat_part(1, core, p),
            lat_part(0, core, p),
            h_send.at[0, p],
            h_recv.at[0, p],
            {"sp": lax.rem(s + 1, S)},
        )

    def to_prev(p):
        return remote(
            lat_part(1, core, p),
            lat_part(2, core, p),
            h_send.at[1, p],
            h_recv.at[1, p],
            {"sp": lax.rem(s + S - 1, S)},
        )

    def halo_start(p):
        send(s < S - 1, to_next(p))
        send(s > 0, to_prev(p))

    halo_start(0)

    def units_of(k):
        if k < 0:
            return [(d - 1, z * Y + lax.rem(y + Y - d, Y), None) for d in range(1, Y)]
        units = []
        for way in range(2):
            at = z - 1 - k if way == 0 else z + 1 + k
            have = at >= 0 if way == 0 else at <= Z - 1
            for u in range(Y):
                units.append((Y - 1 + (k * 2 + way) * Y + u, at * Y + lax.rem(y + u, Y), have))
        return units

    def share(unit):
        n, b, have = unit
        mine = ctx_slice(b, t)
        for d in range(1, X):
            send(
                have,
                remote(
                    mine,
                    mine,
                    x_send.at[n * (X - 1) + d - 1] if X > 1 else None,
                    x_recv.at[n * (X - 1) + d - 1] if X > 1 else None,
                    {"tp": lax.rem(xi + d, X) * 2 + core},
                ),
            )
        send(have, remote(mine, mine, d_send.at[n * X], d_recv.at[n * X], partner))

    def own_arrive(k):
        for n, b, have in units_of(k):
            ref = ctx_slice(b, t)
            if k < 0:
                arrive(None, remote(ref, ref, y_send.at[n], y_recv.at[n], partner))
                u = Y - 1 - n
                if Z > 1:
                    send(*chain(0, 0, u))
                    send(*chain(1, 0, u))
            else:
                way, u = ((n - (Y - 1)) // Y) % 2, (n - (Y - 1)) % Y
                arrive(
                    have,
                    remote(ref, ref, z_send.at[way, k, u], z_recv.at[way, k, u], partner),
                )
                if k + 1 < Z - 1:
                    send(*chain(way, k + 1, u))
            share((n, b, have))

    def x_arrive(k):
        for n, b, have in units_of(k):
            for d in range(1, X):
                ref = ctx_slice(b, lax.rem(xi + X - d, X) * 2 + core)
                at = n * (X - 1) + d - 1
                arrive(have, remote(ref, ref, x_send.at[at], x_recv.at[at], partner))
                send(
                    have, remote(ref, ref, d_send.at[n * X + d], d_recv.at[n * X + d], partner)
                )

    def mate_arrive(k):
        for n, b, have in units_of(k):
            for d in range(X):
                ref = ctx_slice(b, lax.rem(xi + X - d, X) * 2 + 1 - core)
                arrive(have, remote(ref, ref, d_send.at[n * X + d], d_recv.at[n * X + d], partner))

    def hidden(src, first, count, kind):
        step = 32

        @pl.loop(0, count // step, unroll=min(4, count // step))
        def _(i):
            at = pl.ds(pl.multiple_of(first + i * step, step), step)
            v = src[at, :].astype(F32)
            inv = lax.rsqrt(jnp.mean(v * v, axis=-1, keepdims=True) + EPSILON)
            v = v * inv * modrow[2 + kind : 3 + kind, :] + modrow[kind : kind + 1, :]
            hid[pl.ds(pl.multiple_of(i * step, step), step), :] = v.astype(BF16)

    def project(count, dst, first, tiles, start):
        @pl.loop(0, tiles)
        def _(i):
            at = pl.ds(pl.multiple_of(i * TILE, TILE), TILE)
            wat = pl.ds(pl.multiple_of(start + i * TILE, TILE), TILE)
            dst[pl.ds(first, count), at] = dot(hid[0:count, :], wall[:, wat]).astype(BF16)

    def ctx_project(at):
        count = Y * n_ctx
        first = pl.multiple_of(at * count, count)
        hidden(ctx, first, count, 1)
        project(count, ckv, first, 2 * cols // TILE, 0)

    def process(k):
        mate_arrive(k)
        if k < 0:
            ctx_project(z)
        else:

            @pl.when(z - 1 - k >= 0)
            def _():
                ctx_project(z - 1 - k)

            @pl.when(z + 1 + k <= Z - 1)
            def _():
                ctx_project(z + 1 + k)

    own_arrive(-1)
    halo_start(1)

    lane = lax.broadcasted_iota(jnp.int32, (GRID_W, 2 * GRID_W), 1) % GRID_W
    row = lax.broadcasted_iota(jnp.int32, (GRID_W, 2 * GRID_W), 0)
    first = jnp.clip(row - WIN_COLS // 2, 0, GRID_W - WIN_COLS)
    inside = (lane >= first) & (lane < first + WIN_COLS)
    pairs = table.shape[1]

    @pl.loop(0, heads)
    def _(h):
        for p in range(pairs):
            line = jnp.broadcast_to(table_rows[h, p : p + 1, :], (GRID_W, 2 * GRID_W))
            rolled = pltpu.roll(
                line, 2 * GRID_W - (WIN_COLS - 1), 1, stride=1, stride_axis=0
            )
            table[h, p] = jnp.where(inside, rolled, MASKED)

    modbuf[s] = part[...]
    for copy in a_copies:
        copy.wait()
    modfull[t] = jnp.sum(modbuf[...], axis=0)
    b_copies = []
    for d in range(1, T):
        copy = remote(
            modfull.at[t],
            modfull.at[t],
            b_send.at[d - 1],
            b_recv.at[d - 1],
            {"tp": lax.rem(t + d, T)},
        )
        copy.start()
        b_copies.append(copy)

    if Z > 1:
        own_arrive(0)
    halo_start(2)
    x_arrive(-1)
    for copy in b_copies:
        copy.wait()
    for j in range(T):
        at = slice(j * cols, (j + 1) * cols)
        modrow[:, at] = modfull[j]
        modrow[2:4, at] = gain_pre[:, at] * (1.0 + modfull[j, 2:4])

    for i in range(5, 9):
        loads[i].wait()
    hidden(lat, tokens, tokens, 0)
    project(tokens, kv, tokens, 2 * cols // TILE, 0)
    if Z > 2:
        own_arrive(1)
    halo_start(3)
    project(tokens, qg, 0, 2 * cols // TILE, 2 * cols)

    def halo_share():
        for p in range(PIECES):
            arrive(s > 0, to_next(p))
            mine = lat_part(0, core, p)
            send(s > 0, remote(mine, mine, m_send.at[p], m_recv.at[p], partner))
            arrive(s < S - 1, to_prev(p))
            mine = lat_part(2, core, p)
            n = PIECES + p
            send(s < S - 1, remote(mine, mine, m_send.at[n], m_recv.at[n], partner))

    for k in range(1, Z - 1):
        if k > 1:
            own_arrive(k)
        x_arrive(k - 1)
        process(k - 2)
    if Z > 1:
        x_arrive(Z - 2)
        if Z > 2:
            process(Z - 3)
    halo_share()
    if Z > 1:
        process(Z - 2)
    else:
        process(-1)

    @pl.when(s > 0)
    def _():
        for p in range(PIECES):
            ref = lat_part(0, 1 - core, p)
            remote(ref, ref, m_send.at[p], m_recv.at[p], partner).wait_recv()
        hidden(lat, 0, tokens, 0)
        project(tokens, kv, 0, 2 * cols // TILE, 0)

    @pl.when(s < S - 1)
    def _():
        for p in range(PIECES):
            ref = lat_part(2, 1 - core, p)
            remote(ref, ref, m_send.at[PIECES + p], m_recv.at[PIECES + p], partner).wait_recv()
        hidden(lat, 2 * tokens, tokens, 0)
        project(tokens, kv, 2 * tokens, 2 * cols // TILE, 0)

    total_rows = rows * S
    half = lax.broadcasted_iota(jnp.int32, (tokens, 128), 1) < 64
    scale = 0.125

    @pl.loop(0, heads // 2)
    def _(hp):
        at = pl.ds(pl.multiple_of(hp * 128, 128), 128)
        vat = pl.ds(pl.multiple_of(cols + hp * 128, 128), 128)
        q2 = qg[:, at].astype(F32) * scale
        ck = ckv[:, at]
        cv = ckv[:, vat]
        outs = []
        for e in range(2):
            q = jnp.where(half if e == 0 else jnp.logical_not(half), q2, 0.0).astype(BF16)
            sc = dot_t(q, ck)
            sw = []
            bands = []
            for r in range(rows):
                g = s * rows + r
                rs = jnp.clip(g - WIN_ROWS // 2, 0, total_rows - WIN_ROWS)
                band = pl.ds(
                    pl.multiple_of((rs - s * rows + rows) * GRID_W, GRID_W), WIN_ROWS * GRID_W
                )
                bands.append(band)
                bias = jnp.concatenate(
                    [
                        table[hp * 2 + e, rs - g + WIN_ROWS - 1 + 2 * p]
                        for p in range(WIN_ROWS // 2)
                    ],
                    axis=1,
                )
                sw.append(dot_t(q[r * GRID_W : (r + 1) * GRID_W], kv[band, at]) + bias)
            sw = jnp.concatenate(sw, axis=0)
            m = jnp.maximum(
                jnp.max(sc, axis=-1, keepdims=True), jnp.max(sw, axis=-1, keepdims=True)
            )
            pc = jnp.exp(sc - m)
            pw = jnp.exp(sw - m)
            total = jnp.sum(pc, axis=-1, keepdims=True) + jnp.sum(pw, axis=-1, keepdims=True)
            pw = pw.astype(BF16)
            o = dot(pc.astype(BF16), cv)
            ow = [
                dot(pw[r * GRID_W : (r + 1) * GRID_W], kv[bands[r], vat]) for r in range(rows)
            ]
            outs.append((o + jnp.concatenate(ow, axis=0)) / total)
        o = jnp.where(half, outs[0], outs[1])
        gate = qg[:, vat].astype(F32)
        gated[:, at] = (gate / (1.0 + jnp.exp(-gate)) * o).astype(BF16)

    loads[9].wait()
    own = tokens // T
    groups = 4
    span = width // groups
    m_copies = []
    for g in range(groups):
        span_at = pl.ds(g * span, span)
        prod[:, span_at] = dot(gated[...], wo[:, span_at]).astype(BF16)
        copies = []
        for i in range(X):
            n = g * X + i
            copy = remote(
                prod.at[
                    pl.ds(pl.multiple_of((i * 2 + 1 - core) * own, own), own), span_at
                ],
                mate.at[i, :, span_at],
                m_send.at[2 * PIECES + n],
                m_recv.at[2 * PIECES + n],
                partner,
            )
            copy.start()
            copies.append(copy)
        m_copies.append(copies)
    r_copies = []
    for g in range(groups):
        span_at = pl.ds(g * span, span)
        for copy in m_copies[g]:
            copy.wait()
        copies = []
        for i in range(X):
            at = pl.ds(pl.multiple_of((i * 2 + core) * own, own), own)
            pair[i, :, span_at] = (
                prod[at, span_at].astype(F32) + mate[i, :, span_at].astype(F32)
            )
            if X > 1:
                prod[at, span_at] = pair[i, :, span_at].astype(BF16)
        for d in range(1, X):
            other = lax.rem(xi + d, X)
            n = g * (X - 1) + d - 1
            copy = remote(
                prod.at[pl.ds(pl.multiple_of((other * 2 + core) * own, own), own), span_at],
                terms.at[d - 1, :, span_at],
                r_send.at[n],
                r_recv.at[n],
                {"tp": other * 2 + core},
            )
            copy.start()
            copies.append(copy)
        r_copies.append(copies)
    for copies in r_copies:
        for copy in copies:
            copy.wait()
    total = pair[xi]
    for d in range(1, X):
        total = total + terms[d - 1].astype(F32)
    b = total.astype(BF16).astype(F32)
    inv = lax.rsqrt(jnp.mean(b * b, axis=-1, keepdims=True) + EPSILON)
    own_at = pl.ds(pl.multiple_of(tokens + t * own, own), own)
    out[...] = (
        lat[own_at, :].astype(F32) + modrow[4:5, :] * (b * inv * gain_post[...])
    ).astype(BF16)

    for cond, copy in pending:
        if cond is None:
            copy.wait_send()
        else:

            @pl.when(cond)
            def _(copy=copy):
                copy.wait_send()


def layout_of(S, T):
    X = T // 2
    Y = X if S % X == 0 else 1
    return X, Y, S // Y


def shards(
    S,
    T,
    latent,
    context,
    condition,
    context_condition,
    gain_pre,
    gain_post,
    w_shift,
    w_scale,
    w_gate,
    w_query,
    w_key,
    w_value,
    w_silu,
    offset_bias,
    w_out,
):
    in_rows, cols = w_shift.shape
    tokens, width = latent.shape
    n_ctx = context.shape[0]
    heads = offset_bias.shape[0]
    stacked = jnp.stack([condition, context_condition])
    own = lax.dynamic_slice_in_dim(stacked, lax.axis_index("sp") * in_rows, in_rows, 1)
    active = jnp.pad(jax.nn.silu(own.astype(F32)).astype(BF16), ((0, 14), (0, 0)))
    wide = jnp.pad(offset_bias, ((0, 0), (0, 0), (0, GRID_W - offset_bias.shape[2])))
    table_rows = jnp.concatenate([wide[:, :-1], wide[:, 1:]], axis=-1)
    pairs = table_rows.shape[1]
    own_rows = tokens // T
    vmem = pl.BlockSpec(memory_space=pltpu.VMEM)
    hbm = pl.BlockSpec(memory_space=pl.ANY)
    sem = pltpu.SemaphoreType.DMA
    X, Y, Z = layout_of(S, T)
    units = Y - 1 + 2 * (Z - 1) * Y
    return pl.pallas_call(
        functools.partial(kernel, S, T),
        out_shape=jax.ShapeDtypeStruct((own_rows, width), BF16),
        in_specs=[vmem] * 4 + [hbm] * 10,
        out_specs=vmem,
        scratch_shapes=[
            pltpu.VMEM((3 * tokens, width), BF16),
            pltpu.VMEM((S * n_ctx, width), BF16),
            pltpu.VMEM((3, in_rows, cols), BF16),
            pltpu.VMEM((width, 4 * cols), BF16),
            pltpu.VMEM((cols, width), BF16),
            pltpu.VMEM((8, cols), F32),
            pltpu.VMEM((S, 8, cols), F32),
            pltpu.VMEM((T, 8, cols), F32),
            pltpu.VMEM((8, width), F32),
            pltpu.VMEM((max(tokens, Y * n_ctx), width), BF16),
            pltpu.VMEM((tokens, 2 * cols), BF16),
            pltpu.VMEM((3 * tokens, 2 * cols), BF16),
            pltpu.VMEM((S * n_ctx, 2 * cols), BF16),
            pltpu.VMEM((heads, pairs, GRID_W, 2 * GRID_W), F32),
            pltpu.VMEM((tokens, cols), BF16),
            pltpu.VMEM((tokens, width), BF16),
            pltpu.VMEM((X, own_rows, width), F32),
            pltpu.VMEM((X, own_rows, width), BF16),
            pltpu.VMEM((max(X - 1, 1), own_rows, width), BF16),
            sem((10,)),
            sem((max(S - 1, 1),)),
            sem((max(S - 1, 1),)),
            sem((max(T - 1, 1),)),
            sem((max(T - 1, 1),)),
            sem((max(Y - 1, 1),)),
            sem((max(Y - 1, 1),)),
            sem((2, max(Z - 1, 1), Y)),
            sem((2, max(Z - 1, 1), Y)),
            sem((max(units * (X - 1), 1),)),
            sem((max(units * (X - 1), 1),)),
            sem((max(units * X, 1),)),
            sem((max(units * X, 1),)),
            sem((2, PIECES)),
            sem((2, PIECES)),
            sem((2 * PIECES + 4 * X,)),
            sem((2 * PIECES + 4 * X,)),
            sem((4 * max(X - 1, 1),)),
            sem((4 * max(X - 1, 1),)),
        ],
        compiler_params=pltpu.CompilerParams(
            collective_id=0, has_side_effects=True, vmem_limit_bytes=60 * 1024 * 1024
        ),
    )(
        active,
        gain_pre.reshape(1, width),
        gain_post.reshape(1, width),
        table_rows,
        latent,
        context,
        w_shift,
        w_scale,
        w_gate,
        w_query,
        w_key,
        w_value,
        w_silu,
        w_out,
    )


def solution(mesh):
    in_specs = (
        P("sp", None),
        P("sp", None),
        P(),
        P(),
        P(),
        P(),
        P("sp", "tp"),
        P("sp", "tp"),
        P("sp", "tp"),
        P(None, "tp"),
        P(None, "tp"),
        P(None, "tp"),
        P(None, "tp"),
        P("tp", None, None),
        P("tp", None),
    )
    return jax.shard_map(
        functools.partial(shards, mesh.shape["sp"], mesh.shape["tp"]),
        mesh=mesh,
        in_specs=in_specs,
        out_specs=P(("sp", "tp"), None),
        check_vma=False,
    )
```
